32 devices in a mesh: fs: 4 (over y, x), tp: 8 (over z, core).
Axes of the slice: x: 2, y: 2, z: 4, core: 2. Of those that a mesh axis runs over, the one named last changes fastest.
Arguments:
- prompt: bfloat16 [4096, 2048], P(('fs', 'tp')), may hold values from -6 to 6
- norm_gain: float32 [2048], P('tp'), may hold values from 0.1 to 1.9
- gate_master: float32 [8, 2, 512, 2048], P(None, None, 'fs', 'tp'), may hold values from -0.125 to 0.125
- up_master: float32 [8, 2, 512, 2048], P(None, None, 'fs', 'tp'), may hold values from -0.125 to 0.125
- down_master: float32 [8, 2, 512, 2048], P(None, None, 'fs', 'tp'), may hold values from -0.25 to 0.25
- group_pick: int32 [4096, 1], P(('fs', 'tp')), may hold values from 0 to 7; in each aligned block of 128 rows (0 to 127, 128 to 255, ...) at most 32 rows name the same one
- route_weight: bfloat16 [4096, 2], P(('fs', 'tp')), may hold values from 0.099609375 to 1
Outputs:
- gate_serve: bfloat16 [8, 2, 512, 2048], P('tp', None, 'fs')
- up_serve: bfloat16 [8, 2, 512, 2048], P('tp', None, 'fs')
- down_serve: bfloat16 [8, 2, 512, 2048], P('tp', None, 'fs')
- mixed: bfloat16 [4096, 2048], P(('fs', 'tp'))
The draws below stay inside these ranges and needn't reach their ends.
Inputs may be any that keep to these rules, and one draw needn't show every extreme that they name: `group_pick`: in the rows of one device no group is named by more than 32 rows, and in every draw some device's rows name one group exactly 32 times.
All inputs are finite; a program needn't handle non-finite values.
Results may differ from the reference program's by a relative error of at most 0.0081.
Values may be sent and summed in bfloat16 or wider, within the bound.
A program may use at most 64 MiB of HBM per device.

```python
import math
import jax
import jax.numpy as jnp
import numpy as np
from jax import lax

D = 2048
HID = 512
EXP_GRP = 2
TOK_DEV = 128
GROUPS = 8
CAP = 32
TOKENS = 4096


def steps_of(key, shape, shards, smallest, high):
    gain = 1.0
    for position, shards_of in shards:
        heights = jax.random.uniform(jax.random.fold_in(jax.random.fold_in(key, 6), position), (shards_of,), jnp.float32, smallest / len(shards), high / len(shards))
        gain = gain * jnp.repeat(jnp.exp(heights), shape[position] // shards_of).reshape((-1,) + (1,) * (len(shape) - 1 - position))
    return gain


def assign_block(rng, own, number, rows, number_of, top, bound, skew):
    ranking = jax.random.permutation(rng, number_of)
    packed, ordinary = load_shares(number_of, rows * top, bound, skew, True), load_shares(number_of, rows * top, bound, skew, False)
    places = jnp.arange(number_of)

    def named(sizes, rotation):
        used = int((sizes > 0).sum())
        fixed = max(1, used // 4)
        passed = fixed + (places - fixed + rotation * (used - fixed)) % max(1, number_of - fixed)
        return jnp.zeros((number_of,), jnp.int32).at[ranking[jnp.where(places < fixed, places, passed)]].set(jnp.asarray(sizes, jnp.int32))

    sizes = jnp.where(number % 4 == 0, named(packed, number // 4), named(ordinary, number - number // 4 - 1))
    mixed = jax.random.permutation(jax.random.fold_in(own, 3), number_of)
    source_of, taker = mixed[0:number_of // 2 * 2:2], mixed[1:number_of // 2 * 2:2]
    slack = jnp.minimum(sizes[source_of] - 1, bound - sizes[taker]) // 2
    slack = jnp.where((source_of == ranking[0]) | (taker == ranking[0]) | (sizes[taker] == 0), 0, jnp.maximum(slack, 0))
    passed = jax.random.randint(jax.random.fold_in(own, 4), (number_of // 2,), 0, 1 << 20) % (slack + 1)
    sizes = sizes.at[source_of].add(-passed).at[taker].add(passed)
    items = jnp.searchsorted(jnp.cumsum(sizes), jnp.arange(rows * top), side="right").astype(jnp.int32)
    grid = items.reshape(top, rows).T
    grid = grid[jax.random.permutation(jax.random.fold_in(own, 1), rows)]
    rotation = jax.random.randint(jax.random.fold_in(own, 2), (rows, 1), 0, top)
    return jnp.take_along_axis(grid, (jnp.arange(top)[None, :] + rotation) % top, axis=1)


def load_shares(amount, total, reach, skew, full):
    loads = [(1 << 20) // math.isqrt(standing ** skew) + 1 for standing in range(1, amount + 1)]
    largest = reach if full else min(reach, max(-(-total // amount), total * loads[0] // sum(loads)))
    least = 1 if total - largest >= amount - 1 else 0
    given, surplus = [largest] + [least] * (amount - 1), total - largest - least * (amount - 1)
    while surplus > 0:
        movable = [i for i in range(1, amount) if given[i] < largest] or [i for i in range(1, amount) if given[i] < reach]
        whole, budget = sum([loads[i] for i in movable]), surplus
        for i in movable:
            addition = min(reach - given[i], max(1, budget * loads[i] // whole), surplus)
            given[i] = given[i] + addition
            surplus = surplus - addition
    return np.array(given)


def normal_values(own_key, dims, spread, limit, pieces=(), kind=jnp.bfloat16):
    entries = spread * jax.random.normal(own_key, dims, jnp.float32)
    if pieces:
        entries = entries * steps_of(own_key, dims, pieces, -0.22, 0.18)
    return jnp.clip(entries, -limit, limit).astype(kind)


def setup_inputs(seed: int = 0) -> dict:
    splits = jax.random.split(jax.random.key(seed), 8)
    prompt = normal_values(splits[0], (TOKENS, D), 1.0, 6.0, ((0, 32),))
    norm_gain = jnp.clip(1.0 + 0.18 * jax.random.normal(splits[1], (D,), jnp.float32), 0.1, 1.9)
    gate_master = normal_values(splits[2], (GROUPS, EXP_GRP, HID, D), D ** -0.5, 0.125, ((2, 4), (3, 8)), jnp.float32)
    up_master = normal_values(splits[3], (GROUPS, EXP_GRP, HID, D), D ** -0.5, 0.125, ((2, 4), (3, 8)), jnp.float32)
    down_master = normal_values(splits[4], (GROUPS, EXP_GRP, HID, D), HID ** -0.5, 0.25, ((2, 4), (3, 8)), jnp.float32)
    group_pick_keys = jax.random.split(jax.random.fold_in(splits[5], 1), TOKENS // TOK_DEV)
    group_pick_turns = jax.random.permutation(jax.random.fold_in(splits[5], 3), TOKENS // TOK_DEV)
    group_pick = jax.vmap(lambda own, number: assign_block(jax.random.fold_in(splits[5], 2), own, number, TOK_DEV, GROUPS, 1, CAP, 2))(group_pick_keys, group_pick_turns).reshape((TOKENS, 1))
    route_weight = jnp.clip(jnp.exp(math.log(1.0) - 2.306499 * jax.random.uniform(splits[6], (TOKENS, EXP_GRP), jnp.float32) ** steps_of(splits[6], (TOKENS, EXP_GRP), ((0, 32),), -0.2, 0.2)), 0.099609375, 1.0).astype(jnp.bfloat16)
    return dict(prompt=prompt, norm_gain=norm_gain, gate_master=gate_master, up_master=up_master, down_master=down_master, group_pick=group_pick, route_weight=route_weight)


EPS = 1e-06

def reference(prompt, norm_gain, gate_master, up_master, down_master, group_pick, route_weight):
    gate_serve = (gate_master * norm_gain).astype(jnp.bfloat16)
    up_serve = (up_master * norm_gain).astype(jnp.bfloat16)
    down_serve = down_master.astype(jnp.bfloat16)
    values = prompt.astype(jnp.float32)
    normed = (values * lax.rsqrt(lax.optimization_barrier(jnp.mean(values * values, axis=1, keepdims=True)) + EPS)).astype(jnp.bfloat16)
    chosen = group_pick[:, 0].astype(jnp.int32)
    order = jnp.argsort(chosen, stable=True).astype(jnp.int32)
    member = (chosen[:, None] == jnp.arange(GROUPS, dtype=jnp.int32)[None, :]).astype(jnp.int32)
    counts = lax.optimization_barrier(jnp.sum(member, axis=0)).astype(jnp.int32)
    starts = (jnp.cumsum(counts) - counts).astype(jnp.int32)
    row_bound = CAP * (TOKENS // TOK_DEV)
    slot_ids = jnp.arange(row_bound, dtype=jnp.int32)

    def one_group(running, group_index):
        slot_place = jnp.minimum(starts[group_index] + slot_ids, TOKENS - 1).astype(jnp.int32)
        token_ids = order[slot_place].astype(jnp.int32)
        is_valid = slot_ids < counts[group_index]
        group_rows = normed[token_ids].astype(jnp.float32)
        weights = jnp.where(is_valid[:, None], route_weight[token_ids].astype(jnp.float32), 0.0)
        gate_pre = jnp.einsum('sd,ehd->seh', group_rows, gate_serve[group_index].astype(jnp.float32))
        up_pre = jnp.einsum('sd,ehd->seh', group_rows, up_serve[group_index].astype(jnp.float32))
        hidden = (weights[:, :, None] * (jax.nn.silu(gate_pre) * up_pre)).astype(jnp.bfloat16)
        expert_out = jnp.einsum('seh,ehd->sd', hidden.astype(jnp.float32), down_serve[group_index].astype(jnp.float32)).astype(jnp.bfloat16)
        expert_out = jnp.where(is_valid[:, None], expert_out, jnp.zeros_like(expert_out))
        running = running.at[token_ids].add(expert_out)
        return (running, None)
    mixed, _ = lax.scan(one_group, jnp.zeros((TOKENS, D), jnp.bfloat16), jnp.arange(GROUPS, dtype=jnp.int32))
    return (gate_serve, up_serve, down_serve, mixed)
```

```python
import functools

import jax
import jax.numpy as jnp
from jax import lax
from jax.experimental import pallas as pl
from jax.experimental.pallas import tpu as pltpu
from jax.sharding import PartitionSpec as P

EPS = 1e-06
MESH = pl.DeviceIdType.MESH
LANES = 128


def expert_rows(group_rows, weights, pieces):
    gate_piece, up_piece, down_piece = pieces
    expert_count = gate_piece.shape[1]
    unit_count = gate_piece.shape[2]
    model_width = gate_piece.shape[3]
    row_count = group_rows.shape[0]
    gate_matrix = gate_piece.reshape(expert_count * unit_count, model_width)
    up_matrix = up_piece.reshape(expert_count * unit_count, model_width)
    down_matrix = down_piece.reshape(expert_count * unit_count, model_width)
    gate_pre = jnp.einsum("sd,hd->sh", group_rows, gate_matrix, preferred_element_type=jnp.float32)
    up_pre = jnp.einsum("sd,hd->sh", group_rows, up_matrix, preferred_element_type=jnp.float32)
    active = (jax.nn.silu(gate_pre) * up_pre).reshape(row_count, expert_count, unit_count)
    hidden = (weights.astype(jnp.float32)[:, :, None] * active).reshape(
        row_count, expert_count * unit_count
    )
    hidden = hidden.astype(jnp.bfloat16)
    return jnp.dot(hidden, down_matrix, preferred_element_type=jnp.float32)


def flipped(index, mask, size):
    total, bit = 0, 1
    while bit < size:
        digit = lax.rem(lax.div(index, bit), 2)
        total = total + bit * ((1 - digit) if mask & bit else digit)
        bit *= 2
    return total


def exchange_kernel(
    dims,
    gate_in, up_in, down_in, rows_in, placing_ref,
    gate_out, up_out, down_out, mixed_ref,
    xrows, hidden, psend, racc, rsum, ret,
    rows_s, rows_r, w_s, w_r, fwd_s, fwd_r, red_s, red_r, ret_s, ret_r, loc,
):
    fs_n, tp_n, experts, units, width, model, cap = dims
    f = lax.axis_index("fs")
    t = lax.axis_index("tp")
    tp_peer = [flipped(t, k, tp_n) for k in range(tp_n)]
    fs_peer = [flipped(f, j, fs_n) for j in range(fs_n)]

    barrier = pltpu.get_barrier_semaphore()
    for k in range(1, tp_n):
        pl.semaphore_signal(barrier, inc=1, device_id=(f, tp_peer[k]), device_id_type=MESH)
    for j in range(1, fs_n):
        pl.semaphore_signal(barrier, inc=1, device_id=(fs_peer[j], t), device_id_type=MESH)
    pl.semaphore_wait(barrier, tp_n - 1 + fs_n - 1)

    def columns(index):
        return pl.ds(pl.multiple_of(index * width, width), width)

    def remote(src, dst, send, recv, fs_to, tp_to):
        return pltpu.make_async_remote_copy(
            src_ref=src, dst_ref=dst, send_sem=send, recv_sem=recv,
            device_id=(fs_to, tp_to), device_id_type=MESH,
        )

    far_first = list(range(tp_n - 1, 0, -1))
    own_rows = pltpu.make_async_copy(rows_in.at[t], xrows.at[f, t], loc.at[0])
    own_rows.start()
    rows_copy = {}
    for k in far_first:
        rows_copy[k] = remote(
            rows_in.at[tp_peer[k]], xrows.at[f, t], rows_s.at[k], rows_r.at[k], f, tp_peer[k]
        )
        rows_copy[k].start()
    w_copy, own_w = {}, []
    for m, (src, dst) in enumerate(((gate_in, gate_out), (up_in, up_out), (down_in, down_out))):
        own = pltpu.make_async_copy(src.at[t], dst.at[:, columns(t)], loc.at[1 + m])
        own.start()
        own_w.append(own)
        for k in far_first:
            w_copy[m, k] = remote(
                src.at[tp_peer[k]], dst.at[:, columns(t)], w_s.at[m, k], w_r.at[m, k], f, tp_peer[k]
            )
            w_copy[m, k].start()

    fwd_copy = {}
    for k in range(tp_n):
        if k == 0:
            own_rows.wait()
        else:
            rows_copy[k].wait_recv()
        for j in range(fs_n - 1, 0, -1):
            fwd_copy[k, j] = remote(
                xrows.at[f, tp_peer[k]], xrows.at[f, tp_peer[k]],
                fwd_s.at[k, j], fwd_r.at[k, j], fs_peer[j], t,
            )
            fwd_copy[k, j].start()
    for copy in fwd_copy.values():
        copy.wait_recv()
    for m in range(2):
        own_w[m].wait()
        for k in range(1, tp_n):
            w_copy[m, k].wait_recv()

    block = tp_n * cap

    @pl.loop(0, fs_n)
    def _(b):
        tile = xrows[b].reshape(block, model + LANES)
        x = tile[:, :model]
        route = tile[:, model:].astype(jnp.float32)
        nt = (((1,), (1,)), ((), ()))
        gate = lax.dot_general(x, gate_out[...], nt, preferred_element_type=jnp.float32)
        up = lax.dot_general(x, up_out[...], nt, preferred_element_type=jnp.float32)
        active = gate / (1.0 + jnp.exp(-gate)) * up
        for e in range(experts):
            at = slice(e * units, (e + 1) * units)
            hidden[b, :, at] = (route[:, e : e + 1] * active[:, at]).astype(jnp.bfloat16)

    red_copy = {}
    ret_copy = {}

    def reduce_and_return(k):
        col = columns(tp_peer[k])
        total = jnp.dot(hidden[f], down_out[:, col], preferred_element_type=jnp.float32)
        for j in range(1, fs_n):
            red_copy[k, j].wait_recv()
            total = total + racc[k, j].astype(jnp.float32)
        rsum[k] = total.astype(jnp.bfloat16).reshape(tp_n, cap, width)
        for kk in far_first:
            ret_copy[k, kk] = remote(
                rsum.at[k, tp_peer[kk]], ret.at[t, :, col],
                ret_s.at[k, kk], ret_r.at[k, kk], f, tp_peer[kk],
            )
            ret_copy[k, kk].start()
        ret[t, :, col] = rsum[k, t]

    for k in range(tp_n):
        if k == 0:
            own_w[2].wait()
        else:
            w_copy[2, k].wait_recv()
        piece = down_out[:, columns(tp_peer[k])]
        for j in range(fs_n - 1, 0, -1):
            psend[k, j] = jnp.dot(
                hidden[fs_peer[j]], piece, preferred_element_type=jnp.float32
            ).astype(jnp.bfloat16)
        for j in range(fs_n - 1, 0, -1):
            red_copy[k, j] = remote(
                psend.at[k, j], racc.at[k, j], red_s.at[k, j], red_r.at[k, j], fs_peer[j], t
            )
            red_copy[k, j].start()
        if k >= 1:
            reduce_and_return(k - 1)
    reduce_and_return(tp_n - 1)

    for copy in ret_copy.values():
        copy.wait_recv()
    mixed_ref[...] = lax.dot_general(
        placing_ref[...], ret[...].reshape(block, model), (((0,), (0,)), ((), ())),
        preferred_element_type=jnp.float32,
    ).astype(jnp.bfloat16)

    for group in (rows_copy, w_copy, fwd_copy, red_copy, ret_copy):
        for copy in group.values():
            copy.wait_send()


def fused_device(fs_n, gate_local, up_local, down_local, normed, placing, route_weight, capacity):
    tp_n, experts, units, width = gate_local.shape
    tokens, model = normed.shape
    packed = jnp.concatenate(
        [normed, jnp.pad(route_weight, ((0, 0), (0, LANES - route_weight.shape[1])))], axis=1
    )
    rows = jnp.dot(placing, packed, preferred_element_type=jnp.float32).astype(jnp.bfloat16)
    rows = rows.reshape(tp_n, capacity, model + LANES)
    flat = experts * units
    block = tp_n * capacity
    bf16 = jnp.bfloat16
    dma = pltpu.SemaphoreType.DMA
    served = jax.ShapeDtypeStruct((flat, model), bf16)
    vmem = pl.BlockSpec(memory_space=pltpu.VMEM)
    hbm = pl.BlockSpec(memory_space=pl.ANY)
    dims = (fs_n, tp_n, experts, units, width, model, capacity)
    gate_serve, up_serve, down_serve, mixed = pl.pallas_call(
        functools.partial(exchange_kernel, dims),
        out_shape=(served, served, served, jax.ShapeDtypeStruct((tokens, model), bf16)),
        in_specs=[hbm, hbm, hbm, hbm, vmem],
        out_specs=(vmem, vmem, vmem, vmem),
        scratch_shapes=[
            pltpu.VMEM((fs_n, tp_n, capacity, model + LANES), bf16),
            pltpu.VMEM((fs_n, block, flat), bf16),
            pltpu.VMEM((tp_n, fs_n, block, width), bf16),
            pltpu.VMEM((tp_n, fs_n, block, width), bf16),
            pltpu.VMEM((tp_n, tp_n, capacity, width), bf16),
            pltpu.VMEM((tp_n, capacity, model), bf16),
            dma((tp_n,)), dma((tp_n,)),
            dma((3, tp_n)), dma((3, tp_n)),
            dma((tp_n, fs_n)), dma((tp_n, fs_n)),
            dma((tp_n, fs_n)), dma((tp_n, fs_n)),
            dma((tp_n, tp_n)), dma((tp_n, tp_n)),
            dma((4,)),
        ],
        compiler_params=pltpu.CompilerParams(collective_id=0, has_side_effects=True),
    )(
        gate_local.reshape(tp_n, flat, width),
        up_local.reshape(tp_n, flat, width),
        down_local.reshape(tp_n, flat, width),
        rows,
        placing,
    )
    shape = (1, experts, units, model)
    return gate_serve.reshape(shape), up_serve.reshape(shape), down_serve.reshape(shape), mixed


def per_device(prompt, norm_gain, gate_master, up_master, down_master, group_pick, route_weight):
    group_total = lax.axis_size("tp")
    fs_n = lax.axis_size("fs")
    gate_local = (gate_master * norm_gain).astype(jnp.bfloat16)
    up_local = (up_master * norm_gain).astype(jnp.bfloat16)
    down_local = down_master.astype(jnp.bfloat16)
    values = prompt.astype(jnp.float32)
    normed = (values * lax.rsqrt(jnp.mean(values * values, axis=1, keepdims=True) + EPS)).astype(
        jnp.bfloat16
    )
    tok_count = prompt.shape[0]
    capacity = 2 * tok_count // group_total
    slot_total = group_total * capacity
    chosen = group_pick[:, 0]
    member = (chosen[:, None] == jnp.arange(group_total, dtype=jnp.int32)[None, :]).astype(
        jnp.int32
    )
    slot_rank = jnp.sum(jnp.cumsum(member, axis=0) * member, axis=1) - 1
    target = chosen * capacity + slot_rank
    placing = (jnp.arange(slot_total, dtype=jnp.int32)[:, None] == target[None, :]).astype(
        jnp.bfloat16
    )
    width, units = gate_master.shape[3], gate_master.shape[2]
    small = group_total <= 8 and fs_n <= 4
    even = (group_total & (group_total - 1)) == 0 and (fs_n & (fs_n - 1)) == 0
    if small and even and width % LANES == 0 and units % LANES == 0 and capacity % 16 == 0:
        return fused_device(
            fs_n, gate_local, up_local, down_local, normed, placing, route_weight, capacity
        )
    gate_serve, up_serve, down_serve = (
        lax.all_to_all(gate_local, "tp", split_axis=0, concat_axis=3, tiled=True),
        lax.all_to_all(up_local, "tp", split_axis=0, concat_axis=3, tiled=True),
        lax.all_to_all(down_local, "tp", split_axis=0, concat_axis=3, tiled=True),
    )
    send_rows = jnp.dot(placing, normed, preferred_element_type=jnp.float32).astype(jnp.bfloat16)
    send_weights = jnp.dot(placing, route_weight, preferred_element_type=jnp.float32).astype(
        jnp.bfloat16
    )
    got_rows, got_weights = (
        lax.all_to_all(
            send_rows.reshape(group_total, capacity, -1),
            "tp",
            split_axis=0,
            concat_axis=0,
            tiled=True,
        ),
        lax.all_to_all(
            send_weights.reshape(group_total, capacity, -1),
            "tp",
            split_axis=0,
            concat_axis=0,
            tiled=True,
        ),
    )
    group_rows = got_rows.reshape(slot_total, -1)
    weights = got_weights.reshape(slot_total, -1)
    gathered = (
        lax.all_gather(gate_serve, "fs", axis=2, tiled=True),
        lax.all_gather(up_serve, "fs", axis=2, tiled=True),
        lax.all_gather(down_serve, "fs", axis=2, tiled=True),
    )
    summed = expert_rows(group_rows, weights, gathered)
    result = summed.astype(jnp.bfloat16).reshape(group_total, capacity, -1)
    returned = lax.all_to_all(result, "tp", split_axis=0, concat_axis=0, tiled=True)
    mixed = jnp.einsum(
        "st,sd->td", placing, returned.reshape(slot_total, -1), preferred_element_type=jnp.float32
    ).astype(jnp.bfloat16)
    return (gate_serve, up_serve, down_serve, mixed)


def solution(mesh):
    placed = (
        P(("fs", "tp"), None),
        P("tp"),
        P(None, None, "fs", "tp"),
        P(None, None, "fs", "tp"),
        P(None, None, "fs", "tp"),
        P(("fs", "tp"), None),
        P(("fs", "tp"), None),
    )
    return jax.shard_map(
        per_device,
        mesh=mesh,
        in_specs=placed,
        out_specs=(
            P("tp", None, "fs", None),
            P("tp", None, "fs", None),
            P("tp", None, "fs", None),
            P(("fs", "tp"), None),
        ),
        check_vma=False,
    )
```

```python
import functools

import jax
import jax.numpy as jnp
from jax import lax
from jax.experimental import pallas as pl
from jax.experimental.pallas import tpu as pltpu
from jax.sharding import PartitionSpec as P

EPS = 1e-06
MESH = pl.DeviceIdType.MESH
LANES = 128


def expert_rows(group_rows, weights, pieces):
    gate_piece, up_piece, down_piece = pieces
    expert_count = gate_piece.shape[1]
    unit_count = gate_piece.shape[2]
    model_width = gate_piece.shape[3]
    row_count = group_rows.shape[0]
    gate_matrix = gate_piece.reshape(expert_count * unit_count, model_width)
    up_matrix = up_piece.reshape(expert_count * unit_count, model_width)
    down_matrix = down_piece.reshape(expert_count * unit_count, model_width)
    gate_pre = jnp.einsum("sd,hd->sh", group_rows, gate_matrix, preferred_element_type=jnp.float32)
    up_pre = jnp.einsum("sd,hd->sh", group_rows, up_matrix, preferred_element_type=jnp.float32)
    active = (jax.nn.silu(gate_pre) * up_pre).reshape(row_count, expert_count, unit_count)
    hidden = (weights.astype(jnp.float32)[:, :, None] * active).reshape(
        row_count, expert_count * unit_count
    )
    hidden = hidden.astype(jnp.bfloat16)
    return jnp.dot(hidden, down_matrix, preferred_element_type=jnp.float32)


def flipped(index, mask, size):
    total, bit = 0, 1
    while bit < size:
        digit = lax.rem(lax.div(index, bit), 2)
        total = total + bit * ((1 - digit) if mask & bit else digit)
        bit *= 2
    return total


def exchange_kernel(
    dims,
    gate_in, up_in, down_in, rows_in, placing_ref,
    gate_out, up_out, down_out, mixed_ref,
    xrows, hidden, psend, racc, qsend, qacc, rsum, ret,
    rows_s, rows_r, w_s, w_r, fwd_s, fwd_r, red_s, red_r, sec_s, sec_r, ret_s, ret_r, loc,
):
    fs_n, tp_n, experts, units, width, model, cap = dims
    f = lax.axis_index("fs")
    t = lax.axis_index("tp")
    tp_peer = [flipped(t, k, tp_n) for k in range(tp_n)]
    fs_peer = [flipped(f, j, fs_n) for j in range(fs_n)]

    barrier = pltpu.get_barrier_semaphore()
    for k in range(1, tp_n):
        pl.semaphore_signal(barrier, inc=1, device_id=(f, tp_peer[k]), device_id_type=MESH)
    for j in range(1, fs_n):
        pl.semaphore_signal(barrier, inc=1, device_id=(fs_peer[j], t), device_id_type=MESH)
    pl.semaphore_wait(barrier, tp_n - 1 + fs_n - 1)

    def columns(index):
        return pl.ds(pl.multiple_of(index * width, width), width)

    def remote(src, dst, send, recv, fs_to, tp_to):
        return pltpu.make_async_remote_copy(
            src_ref=src, dst_ref=dst, send_sem=send, recv_sem=recv,
            device_id=(fs_to, tp_to), device_id_type=MESH,
        )

    far_first = [1] + list(range(tp_n - 1, 1, -1))
    pieces = [0] + far_first
    own_rows = pltpu.make_async_copy(rows_in.at[t], xrows.at[f, t], loc.at[0])
    own_rows.start()
    rows_copy = {}
    for k in far_first:
        rows_copy[k] = remote(
            rows_in.at[tp_peer[k]], xrows.at[f, t], rows_s.at[k], rows_r.at[k], f, tp_peer[k]
        )
        rows_copy[k].start()
    w_copy, own_w = {}, []
    for m, (src, dst) in enumerate(((gate_in, gate_out), (up_in, up_out), (down_in, down_out))):
        own = pltpu.make_async_copy(src.at[t], dst.at[:, columns(t)], loc.at[1 + m])
        own.start()
        own_w.append(own)
        for k in far_first:
            w_copy[m, k] = remote(
                src.at[tp_peer[k]], dst.at[:, columns(t)], w_s.at[m, k], w_r.at[m, k], f, tp_peer[k]
            )

    fwd_copy = {}
    for k in pieces:
        if k == 0:
            own_rows.wait()
        else:
            rows_copy[k].wait_send()
            w_copy[0, k].start()
            rows_copy[k].wait_recv()
        for j in range(fs_n - 1, 0, -1):
            fwd_copy[k, j] = remote(
                xrows.at[f, tp_peer[k]], xrows.at[f, tp_peer[k]],
                fwd_s.at[k, j], fwd_r.at[k, j], fs_peer[j], t,
            )
            fwd_copy[k, j].start()
    for m in (1, 2):
        for k in far_first:
            w_copy[m - 1, k].wait_send()
            w_copy[m, k].start()
    for copy in fwd_copy.values():
        copy.wait_recv()
    for m in range(2):
        own_w[m].wait()
        for k in range(1, tp_n):
            w_copy[m, k].wait_recv()

    block = tp_n * cap

    @pl.loop(0, fs_n)
    def _(b):
        tile = xrows[b].reshape(block, model + LANES)
        x = tile[:, :model]
        route = tile[:, model:].astype(jnp.float32)
        nt = (((1,), (1,)), ((), ()))
        gate = lax.dot_general(x, gate_out[...], nt, preferred_element_type=jnp.float32)
        up = lax.dot_general(x, up_out[...], nt, preferred_element_type=jnp.float32)
        active = gate / (1.0 + jnp.exp(-gate)) * up
        for e in range(experts):
            at = slice(e * units, (e + 1) * units)
            hidden[b, :, at] = (route[:, e : e + 1] * active[:, at]).astype(jnp.bfloat16)

    first_copy, second_copy, ret_copy = {}, {}, {}
    half = width // 2
    order = ((1, 2), (2, 1))

    def partial(index, k, h):
        at = pl.ds(pl.multiple_of(tp_peer[k] * width + h * half, half), half)
        return jnp.dot(hidden[index], down_out[:, at], preferred_element_type=jnp.float32)

    def first_step(k):
        for h, (a, b) in enumerate(order):
            for n, index in enumerate((fs_peer[a], fs_peer[a ^ b])):
                psend[k, h, n] = partial(index, k, h).astype(jnp.bfloat16)
        for h, (a, b) in enumerate(order):
            first_copy[k, h] = remote(
                psend.at[k, h], racc.at[k, h], red_s.at[k, h], red_r.at[k, h], fs_peer[a], t
            )
            first_copy[k, h].start()

    def second_step(k):
        for h, (a, b) in enumerate(order):
            part = partial(fs_peer[b], k, h)
            first_copy[k, h].wait_recv()
            qsend[k, h] = (part + racc[k, h, 1].astype(jnp.float32)).astype(jnp.bfloat16)
        for h, (a, b) in enumerate(order):
            second_copy[k, h] = remote(
                qsend.at[k, h], qacc.at[k, h], sec_s.at[k, h], sec_r.at[k, h], fs_peer[b], t
            )
            second_copy[k, h].start()

    def reduce_and_return(k):
        col = columns(tp_peer[k])
        for h in range(2):
            total = partial(f, k, h) + racc[k, h, 0].astype(jnp.float32)
            second_copy[k, h].wait_recv()
            total = total + qacc[k, h].astype(jnp.float32)
            rsum[k, :, :, h * half : (h + 1) * half] = total.astype(jnp.bfloat16).reshape(
                tp_n, cap, half
            )
        for kk in far_first:
            ret_copy[k, kk] = remote(
                rsum.at[k, tp_peer[kk]], ret.at[t, :, col],
                ret_s.at[k, kk], ret_r.at[k, kk], f, tp_peer[kk],
            )
            ret_copy[k, kk].start()
        ret[t, :, col] = rsum[k, t]

    for step in range(tp_n + 2):
        if step < tp_n:
            k = pieces[step]
            if k == 0:
                own_w[2].wait()
            else:
                w_copy[2, k].wait_recv()
            first_step(k)
        if 1 <= step <= tp_n:
            second_step(pieces[step - 1])
        if step >= 2:
            reduce_and_return(pieces[step - 2])

    for copy in ret_copy.values():
        copy.wait_recv()
    mixed_ref[...] = lax.dot_general(
        placing_ref[...], ret[...].reshape(block, model), (((0,), (0,)), ((), ())),
        preferred_element_type=jnp.float32,
    ).astype(jnp.bfloat16)

    for k in far_first:
        w_copy[2, k].wait_send()
    for group in (fwd_copy, first_copy, second_copy, ret_copy):
        for copy in group.values():
            copy.wait_send()


def fused_device(fs_n, gate_local, up_local, down_local, normed, placing, route_weight, capacity):
    tp_n, experts, units, width = gate_local.shape
    tokens, model = normed.shape
    packed = jnp.concatenate(
        [normed, jnp.pad(route_weight, ((0, 0), (0, LANES - route_weight.shape[1])))], axis=1
    )
    rows = jnp.dot(placing, packed, preferred_element_type=jnp.float32).astype(jnp.bfloat16)
    rows = rows.reshape(tp_n, capacity, model + LANES)
    flat = experts * units
    block = tp_n * capacity
    bf16 = jnp.bfloat16
    dma = pltpu.SemaphoreType.DMA
    served = jax.ShapeDtypeStruct((flat, model), bf16)
    vmem = pl.BlockSpec(memory_space=pltpu.VMEM)
    hbm = pl.BlockSpec(memory_space=pl.ANY)
    dims = (fs_n, tp_n, experts, units, width, model, capacity)
    gate_serve, up_serve, down_serve, mixed = pl.pallas_call(
        functools.partial(exchange_kernel, dims),
        out_shape=(served, served, served, jax.ShapeDtypeStruct((tokens, model), bf16)),
        in_specs=[hbm, hbm, hbm, hbm, vmem],
        out_specs=(vmem, vmem, vmem, vmem),
        scratch_shapes=[
            pltpu.VMEM((fs_n, tp_n, capacity, model + LANES), bf16),
            pltpu.VMEM((fs_n, block, flat), bf16),
            pltpu.VMEM((tp_n, 2, 2, block, width // 2), bf16),
            pltpu.VMEM((tp_n, 2, 2, block, width // 2), bf16),
            pltpu.VMEM((tp_n, 2, block, width // 2), bf16),
            pltpu.VMEM((tp_n, 2, block, width // 2), bf16),
            pltpu.VMEM((tp_n, tp_n, capacity, width), bf16),
            pltpu.VMEM((tp_n, capacity, model), bf16),
            dma((tp_n,)), dma((tp_n,)),
            dma((3, tp_n)), dma((3, tp_n)),
            dma((tp_n, fs_n)), dma((tp_n, fs_n)),
            dma((tp_n, 2)), dma((tp_n, 2)),
            dma((tp_n, 2)), dma((tp_n, 2)),
            dma((tp_n, tp_n)), dma((tp_n, tp_n)),
            dma((4,)),
        ],
        compiler_params=pltpu.CompilerParams(collective_id=0, has_side_effects=True),
    )(
        gate_local.reshape(tp_n, flat, width),
        up_local.reshape(tp_n, flat, width),
        down_local.reshape(tp_n, flat, width),
        rows,
        placing,
    )
    shape = (1, experts, units, model)
    return gate_serve.reshape(shape), up_serve.reshape(shape), down_serve.reshape(shape), mixed


def per_device(prompt, norm_gain, gate_master, up_master, down_master, group_pick, route_weight):
    group_total = lax.axis_size("tp")
    fs_n = lax.axis_size("fs")
    gate_local = (gate_master * norm_gain).astype(jnp.bfloat16)
    up_local = (up_master * norm_gain).astype(jnp.bfloat16)
    down_local = down_master.astype(jnp.bfloat16)
    values = prompt.astype(jnp.float32)
    normed = (values * lax.rsqrt(jnp.mean(values * values, axis=1, keepdims=True) + EPS)).astype(
        jnp.bfloat16
    )
    tok_count = prompt.shape[0]
    capacity = 2 * tok_count // group_total
    slot_total = group_total * capacity
    chosen = group_pick[:, 0]
    member = (chosen[:, None] == jnp.arange(group_total, dtype=jnp.int32)[None, :]).astype(
        jnp.int32
    )
    slot_rank = jnp.sum(jnp.cumsum(member, axis=0) * member, axis=1) - 1
    target = chosen * capacity + slot_rank
    placing = (jnp.arange(slot_total, dtype=jnp.int32)[:, None] == target[None, :]).astype(
        jnp.bfloat16
    )
    width, units = gate_master.shape[3], gate_master.shape[2]
    small = group_total in (4, 8) and fs_n == 4
    if small and width % (2 * LANES) == 0 and units % LANES == 0 and capacity % 16 == 0:
        return fused_device(
            fs_n, gate_local, up_local, down_local, normed, placing, route_weight, capacity
        )
    gate_serve, up_serve, down_serve = (
        lax.all_to_all(gate_local, "tp", split_axis=0, concat_axis=3, tiled=True),
        lax.all_to_all(up_local, "tp", split_axis=0, concat_axis=3, tiled=True),
        lax.all_to_all(down_local, "tp", split_axis=0, concat_axis=3, tiled=True),
    )
    send_rows = jnp.dot(placing, normed, preferred_element_type=jnp.float32).astype(jnp.bfloat16)
    send_weights = jnp.dot(placing, route_weight, preferred_element_type=jnp.float32).astype(
        jnp.bfloat16
    )
    got_rows, got_weights = (
        lax.all_to_all(
            send_rows.reshape(group_total, capacity, -1),
            "tp",
            split_axis=0,
            concat_axis=0,
            tiled=True,
        ),
        lax.all_to_all(
            send_weights.reshape(group_total, capacity, -1),
            "tp",
            split_axis=0,
            concat_axis=0,
            tiled=True,
        ),
    )
    group_rows = got_rows.reshape(slot_total, -1)
    weights = got_weights.reshape(slot_total, -1)
    gathered = (
        lax.all_gather(gate_serve, "fs", axis=2, tiled=True),
        lax.all_gather(up_serve, "fs", axis=2, tiled=True),
        lax.all_gather(down_serve, "fs", axis=2, tiled=True),
    )
    summed = expert_rows(group_rows, weights, gathered)
    result = summed.astype(jnp.bfloat16).reshape(group_total, capacity, -1)
    returned = lax.all_to_all(result, "tp", split_axis=0, concat_axis=0, tiled=True)
    mixed = jnp.einsum(
        "st,sd->td", placing, returned.reshape(slot_total, -1), preferred_element_type=jnp.float32
    ).astype(jnp.bfloat16)
    return (gate_serve, up_serve, down_serve, mixed)


def solution(mesh):
    placed = (
        P(("fs", "tp"), None),
        P("tp"),
        P(None, None, "fs", "tp"),
        P(None, None, "fs", "tp"),
        P(None, None, "fs", "tp"),
        P(("fs", "tp"), None),
        P(("fs", "tp"), None),
    )
    return jax.shard_map(
        per_device,
        mesh=mesh,
        in_specs=placed,
        out_specs=(
            P("tp", None, "fs", None),
            P("tp", None, "fs", None),
            P("tp", None, "fs", None),
            P(("fs", "tp"), None),
        ),
        check_vma=False,
    )
```
